32 devices in a mesh: grp: 2 (over y), row: 4 (over z), col: 4 (over x, core).
Axes of the slice: x: 2, y: 2, z: 4, core: 2. Of those that a mesh axis runs over, the one named last changes fastest.
Arguments:
- tokens: bfloat16 [5120, 2048], P(('grp', 'row')), parts along dimension 0, may hold values from -6 to 6
- w_four: bfloat16 [2048, 1024], P(None, 'col'), may hold values from -0.125 to 0.125
- w_gate: bfloat16 [2048, 2048], P(None, 'col'), may hold values from -0.125 to 0.125
- w_back: bfloat16 [1024, 2048], P(None, 'col'), may hold values from -0.1875 to 0.1875
Outputs:
- mixed: bfloat16 [5120, 2048], P(('grp', 'row'), 'col'), parts along dimension 0
The draws below stay inside these ranges and needn't reach their ends.
There are 2 independent parts, one for each index of `grp`. The reference program is written for one: setup_inputs(seed, part) draws one part's arguments, and reference() takes and returns one part's arrays. A program takes and returns all parts, laid end to end along the dimension named above; an argument that names none is the same for every part. Nothing has to cross between parts.
All inputs are finite; a program needn't handle non-finite values.
Results may differ from the reference program's by a relative error of at most 0.0085.
Values may be sent and summed in bfloat16 or wider, within the bound.
A program may use at most 64 MiB of HBM per device.

```python
import jax
import jax.numpy as jnp

D = 2048
GROUP_DIM = 128
FGROUPS = 8
FW = 1024
SEQ = 2560


def shard_levels(rng, shape, shards, low, top_value):
    loudness, own = 1.0, jax.random.fold_in(rng, 6)
    for axis_at, shards_of in shards:
        draws = jnp.exp(jax.random.uniform(jax.random.fold_in(own, axis_at), (shards_of,), jnp.float32, low / len(shards), top_value / len(shards)))
        loudness = loudness * jnp.repeat(draws, shape[axis_at] // shards_of).reshape([-1 if axis == axis_at else 1 for axis in range(len(shape))])
    return loudness


def gaussian(own_key, extent, spread, bound, shards=(), held_as=jnp.bfloat16):
    gain = shard_levels(own_key, extent, shards, -0.22, 0.18) if shards else 1.0
    values = jax.random.normal(own_key, extent, jnp.float32) * spread * gain
    return jnp.minimum(jnp.maximum(values, -bound), bound).astype(held_as)


def setup_inputs(seed: int = 0, part: int = 0) -> dict:
    keys = jax.random.split(jax.random.key(seed), 5)
    part_splits = jax.random.split(jax.random.fold_in(keys[4], part), 5)
    tokens = gaussian(part_splits[0], (SEQ, D), 1.0, 6.0, ((0, 4),))
    w_four = gaussian(keys[1], (D, FW), D ** -0.5, 0.125, ((1, 4),))
    w_gate = gaussian(keys[2], (D, D), D ** -0.5, 0.125, ((1, 4),))
    w_back = gaussian(keys[3], (FW, D), FW ** -0.5, 0.1875, ((1, 4),))
    return dict(tokens=tokens, w_four=w_four, w_gate=w_gate, w_back=w_back)


def reference(tokens, w_four, w_gate, w_back):
    feats = jnp.dot(tokens, w_four, preferred_element_type=jnp.float32).astype(jnp.bfloat16)
    length = feats.shape[0]
    lifted = feats.astype(jnp.float32).reshape(length, FGROUPS, GROUP_DIM)
    spectrum = jnp.real(jnp.fft.fft2(lifted, axes=(0, 2), norm="ortho"))
    four = spectrum.reshape(length, FGROUPS * GROUP_DIM).astype(jnp.bfloat16)
    proj = jnp.dot(four, w_back, preferred_element_type=jnp.float32)
    gate = jax.nn.sigmoid(jnp.dot(tokens, w_gate, preferred_element_type=jnp.float32))
    return (gate * proj).astype(jnp.bfloat16)
```

```python
import functools
import math

import jax
import jax.numpy as jnp
import numpy as np
from jax import lax
from jax.experimental import pallas as pl
from jax.experimental.pallas import tpu as pltpu
from jax.sharding import PartitionSpec as P

GROUP_DIM = 128


def tables(count_len):
    steps = lax.iota(jnp.int32, count_len)
    product = steps[:, None] * steps[None, :] % count_len
    angles = product.astype(jnp.float32) * (2.0 * math.pi / count_len)
    return (jnp.cos(angles), jnp.sin(angles))


def channel_mix(values, matrix):
    height = values.shape[0]
    shaped = values.reshape(height, -1, GROUP_DIM)
    mixed_ch = jnp.einsum("ngc,cj->ngj", shaped, matrix, precision=lax.Precision.HIGHEST)
    return mixed_ch.reshape(height, -1)


def across_rows(values, matrix):
    return jnp.einsum("kr,rmc->kmc", matrix, values, precision=lax.Precision.HIGHEST)


def long_transform(col_re, col_im):
    length = col_re.shape[0]
    first_len = 8
    second_len = length // first_len
    shaped_re = col_re.reshape(first_len, second_len, -1)
    shaped_im = col_im.reshape(first_len, second_len, -1)
    cos_first, sin_first = tables(first_len)
    cos_second, sin_second = tables(second_len)
    section_re = across_rows(shaped_re, cos_first) + across_rows(shaped_im, sin_first)
    section_im = across_rows(shaped_im, cos_first) - across_rows(shaped_re, sin_first)
    outer = lax.iota(jnp.int32, first_len)[:, None]
    inner = lax.iota(jnp.int32, second_len)[None, :]
    angle = (outer * inner % length).astype(jnp.float32) * (2.0 * math.pi / length)
    turn_cos = jnp.cos(angle)[:, :, None]
    turn_sin = jnp.sin(angle)[:, :, None]
    bent_re = section_re * turn_cos + section_im * turn_sin
    bent_im = section_im * turn_cos - section_re * turn_sin
    final_re = jnp.einsum("qb,kbc->qkc", cos_second, bent_re, precision=lax.Precision.HIGHEST)
    final_re = final_re + jnp.einsum(
        "qb,kbc->qkc", sin_second, bent_im, precision=lax.Precision.HIGHEST
    )
    final_re = final_re.reshape(length, -1)
    final_im = jnp.einsum("qb,kbc->qkc", cos_second, bent_im, precision=lax.Precision.HIGHEST)
    final_im = final_im - jnp.einsum(
        "qb,kbc->qkc", sin_second, bent_re, precision=lax.Precision.HIGHEST
    )
    return (final_re, final_im.reshape(length, -1))


def on_device(tokens, w_four, w_gate, w_back):
    length = tokens.shape[0]
    row_count = lax.axis_size("row")
    row_index = lax.axis_index("row")
    piece_rows = length // row_count
    total_len = length * row_count
    feats = jnp.dot(tokens, w_four, preferred_element_type=jnp.float32).astype(jnp.bfloat16)
    lifted = feats.astype(jnp.float32)
    cos_group, sin_group = tables(GROUP_DIM)
    cos_rows, sin_rows = tables(row_count)
    residue = lax.iota(jnp.int32, row_count)[:, None]
    within = row_index * piece_rows + lax.iota(jnp.int32, piece_rows)[None, :]
    twist = (residue * within % total_len).astype(jnp.float32) * (2.0 * math.pi / total_len)
    twist_cos = jnp.cos(twist)[:, :, None]
    twist_sin = jnp.sin(twist)[:, :, None]
    line_re = lax.all_to_all(
        lifted[None].astype(jnp.bfloat16), "row", split_axis=1, concat_axis=0, tiled=True
    ).astype(jnp.float32)
    freq_re = across_rows(line_re, cos_rows)
    freq_im = -across_rows(line_re, sin_rows)
    turned_re = freq_re * twist_cos + freq_im * twist_sin
    turned_im = freq_im * twist_cos - freq_re * twist_sin
    col_re, col_im = (
        lax.all_to_all(turned_re, "row", split_axis=0, concat_axis=1, tiled=True),
        lax.all_to_all(turned_im, "row", split_axis=0, concat_axis=1, tiled=True),
    )
    col_re = col_re.reshape(length, -1)
    col_im = col_im.reshape(length, -1)
    whole_re, whole_im = long_transform(col_re, col_im)
    result = channel_mix(whole_re, cos_group) + channel_mix(whole_im, sin_group)
    scaled = (result * (1.0 / math.sqrt(total_len * GROUP_DIM))).astype(jnp.bfloat16)
    ordered = lax.all_to_all(scaled[:, None], "row", split_axis=0, concat_axis=1, tiled=True)
    ordered = ordered.reshape(length, -1)
    proj = jnp.dot(
        lax.all_gather(ordered, "col", axis=1, tiled=True),
        w_back,
        preferred_element_type=jnp.float32,
    )
    gate = jax.nn.sigmoid(jnp.dot(tokens, w_gate, preferred_element_type=jnp.float32))
    return (gate * proj).astype(jnp.bfloat16)


MESH = pl.DeviceIdType.MESH
TILE = 128


def position_table(length, row_count):
    place = np.arange(length)
    order = place.reshape(-1, row_count).T.reshape(-1)
    angle = 2.0 * np.pi * (np.outer(order, place) % (length * row_count)) / (length * row_count)
    table = np.concatenate([np.cos(angle), np.sin(angle)], axis=1)
    return table.reshape(row_count, length // row_count, 2 * length).astype(jnp.bfloat16)


def group_table():
    step = np.arange(GROUP_DIM)
    angle = 2.0 * np.pi * (np.outer(step, step) % GROUP_DIM) / GROUP_DIM
    return np.concatenate([np.cos(angle), np.sin(angle)], axis=1).astype(jnp.bfloat16)


def dot32(a, b):
    return jnp.dot(a, b, preferred_element_type=jnp.float32)


def mixing_kernel(
    tokens_hbm, four_hbm, gate_hbm, back_hbm, table_hbm, group_hbm, out_ref,
    tokens, w_four, w_gate, w_back, table, group, turned, lines, spect, final, blocks, outer, gate, total,
    load_sem, token_sem, line_send, line_recv, outer_send, outer_recv, col_send, col_recv,
):
    row, col = lax.axis_index("row"), lax.axis_index("col")
    length = tokens.shape[0]
    quarter = length // 4
    tiles = length // TILE
    groups = lines.shape[0]
    scale = 1.0 / math.sqrt(4 * length * GROUP_DIM)
    inner = jnp.logical_or(row == 1, row == 2)
    sibling = col + 1 - 2 * (col % 2)
    across = col + 2 - 4 * (col // 2)

    loads = []
    for at, (source, target) in enumerate(
        ((four_hbm, w_four), (gate_hbm, w_gate), (table_hbm, table), (group_hbm, group), (back_hbm, w_back))
    ):
        loads.append(pltpu.make_async_copy(source, target, load_sem.at[at]))

    def token_copy(tile):
        rows = pl.ds(pl.multiple_of(tile * TILE, TILE), TILE)
        return pltpu.make_async_copy(tokens_hbm.at[rows, :], tokens.at[rows, :], token_sem.at[tile])

    loads[0].start()
    for tile in range(tiles):
        token_copy(tile).start()
    for load in loads[1:]:
        load.start()

    barrier = pltpu.get_barrier_semaphore()
    for step in (1, 2, 3):
        pl.semaphore_signal(barrier, inc=1, device_id={"row": (row + step) % 4}, device_id_type=MESH)
    for peer in (sibling, across):
        pl.semaphore_signal(barrier, inc=1, device_id={"col": peer}, device_id_type=MESH)

    loads[0].wait()

    @pl.loop(0, tiles)
    def _(tile):
        token_copy(tile).wait()
        rows = pl.ds(pl.multiple_of(tile * TILE, TILE), TILE)
        feats = dot32(tokens[rows, :], w_four[...]).astype(jnp.bfloat16)
        for g in range(groups):
            lines[g, row, rows, :] = feats[:, g * GROUP_DIM : (g + 1) * GROUP_DIM]

    pl.semaphore_wait(barrier, 5)

    def line_copy(g, origin, target, at):
        return pltpu.make_async_remote_copy(
            src_ref=lines.at[g, origin],
            dst_ref=lines.at[g, origin],
            send_sem=line_send.at[g, at],
            recv_sem=line_recv.at[g, origin],
            device_id={"row": target},
            device_id_type=MESH,
        )

    for g in range(groups):

        @pl.when(inner)
        def _():
            line_copy(g, row, 3 - row, 0).start()

        @pl.when(jnp.logical_not(inner))
        def _():
            near = 1 + row // 3
            line_copy(g, row, 3 - near, 0).start()
            line_copy(g, row, near, 1).start()

    loads[1].wait()

    @pl.loop(0, tiles)
    def _(tile):
        rows = pl.ds(pl.multiple_of(tile * TILE, TILE), TILE)
        gate[rows, :] = jax.nn.sigmoid(dot32(tokens[rows, :], w_gate[...]))

    for load in loads[2:]:
        load.wait()

    @pl.when(inner)
    def _():
        for at, out_row in enumerate((3 * (row - 1), row)):
            turn = out_row * lax.broadcasted_iota(jnp.int32, (quarter, length), 1) % 4
            for s in range(4):
                cos_at = table[s, :, :length].astype(jnp.float32)
                sin_at = table[s, :, length:].astype(jnp.float32)
                odd, minus = turn % 2 == 1, jnp.where(turn >= 2, -1.0, 1.0)
                turned_cos = jnp.where(odd, -sin_at, cos_at) * minus
                turned_sin = jnp.where(odd, cos_at, sin_at) * minus
                turned[at, s, :, :length] = turned_cos.astype(jnp.bfloat16)
                turned[at, s, :, length:] = (-turned_sin).astype(jnp.bfloat16)

    def outer_copy(g):
        return pltpu.make_async_remote_copy(
            src_ref=outer.at[g],
            dst_ref=blocks.at[g, 0],
            send_sem=outer_send.at[g],
            recv_sem=outer_recv.at[g],
            device_id={"row": 3 * (row // 2)},
            device_id_type=MESH,
        )

    def col_copy(g, source, slot, target):
        return pltpu.make_async_remote_copy(
            src_ref=blocks.at[g, source],
            dst_ref=blocks.at[g, slot],
            send_sem=col_send.at[g, slot],
            recv_sem=col_recv.at[g, slot],
            device_id={"col": target},
            device_id_type=MESH,
        )

    def transform(g):
        for step in (1, 2, 3):
            origin = (row + step) % 4
            pltpu.make_async_copy(lines.at[g, origin], lines.at[g, origin], line_recv.at[g, origin]).wait()

        @pl.loop(0, tiles)
        def _(tile):
            start = pl.multiple_of(tile * TILE, TILE)
            rows, low = pl.ds(start, TILE), pl.ds(pl.multiple_of(length + start, TILE), TILE)
            x0, x1, x2, x3 = (lines[g, at, rows, :].astype(jnp.float32) for at in range(4))
            even, odd = x0 + x2, x1 + x3
            parts = (even + odd, x0 - x2, even - odd, x1 - x3)
            mixed = [dot32(part.astype(jnp.bfloat16), group[...]) for part in parts]
            cos_of = [part[:, :GROUP_DIM] for part in mixed]
            sin_of = [part[:, GROUP_DIM:] for part in mixed]
            for s in (0, 2):
                spect[s, rows, :] = cos_of[s].astype(jnp.bfloat16)
                spect[s, low, :] = sin_of[s].astype(jnp.bfloat16)
            spect[1, rows, :] = (cos_of[1] - sin_of[3]).astype(jnp.bfloat16)
            spect[1, low, :] = (sin_of[1] + cos_of[3]).astype(jnp.bfloat16)
            spect[3, rows, :] = (cos_of[1] + sin_of[3]).astype(jnp.bfloat16)
            spect[3, low, :] = (sin_of[1] - cos_of[3]).astype(jnp.bfloat16)

        for at in range(2):
            for s in range(4):
                final[at, pl.ds(s, quarter, stride=4), :] = dot32(turned[at, s], spect[s]) * scale
            if at == 0:
                outer[g] = final[at].astype(jnp.bfloat16)
                outer_copy(g).start()
            else:
                blocks[g, 0] = final[at].astype(jnp.bfloat16)

    def back_rows(g, peer):
        return w_back[pl.ds(pl.multiple_of((peer * groups + g) * GROUP_DIM, GROUP_DIM), GROUP_DIM), :]

    opposite = across + 1 - 2 * (across % 2)
    for g in range(groups):
        pl.when(inner)(functools.partial(transform, g))

        @pl.when(jnp.logical_not(inner))
        def _():
            outer_copy(g).wait_recv()

        col_copy(g, 0, 2, across).start()
        col_copy(g, 0, 1, sibling).start()
        col_copy(g, 0, 1, sibling).wait_recv()

        @pl.loop(0, tiles)
        def _(tile):
            rows = pl.ds(pl.multiple_of(tile * TILE, TILE), TILE)
            share = dot32(blocks[g, 0, rows, :], back_rows(g, col)) + dot32(
                blocks[g, 1, rows, :], back_rows(g, sibling)
            )
            total[rows, :] = share if g == 0 else total[rows, :] + share

        col_copy(g, 0, 2, across).wait_recv()
        col_copy(g, 2, 3, sibling).start()
        col_copy(g, 2, 3, sibling).wait_recv()

        @pl.loop(0, tiles)
        def _(tile):
            rows = pl.ds(pl.multiple_of(tile * TILE, TILE), TILE)
            share = dot32(blocks[g, 2, rows, :], back_rows(g, across)) + dot32(
                blocks[g, 3, rows, :], back_rows(g, opposite)
            )
            summed = total[rows, :] + share
            if g < groups - 1:
                total[rows, :] = summed
            else:
                out_ref[rows, :] = (gate[rows, :] * summed).astype(jnp.bfloat16)

    for g in range(groups):
        for slot in (1, 2, 3):
            col_copy(g, 0 if slot < 3 else 2, slot, sibling).wait_send()
        line_copy(g, row, 3 - row, 0).wait_send()

        @pl.when(inner)
        def _():
            outer_copy(g).wait_send()

        @pl.when(jnp.logical_not(inner))
        def _():
            line_copy(g, row, 3 - row, 1).wait_send()


def on_line(tokens, w_four, w_gate, w_back):
    length, width = tokens.shape
    groups = w_four.shape[1] // GROUP_DIM
    features = w_gate.shape[1]
    quarter = length // 4
    low = jnp.bfloat16
    table = jnp.asarray(position_table(length, 4))
    group = jnp.asarray(group_table())
    hbm = pl.BlockSpec(memory_space=pl.ANY)
    return pl.pallas_call(
        mixing_kernel,
        out_shape=jax.ShapeDtypeStruct((length, features), low),
        in_specs=[hbm] * 6,
        out_specs=pl.BlockSpec(memory_space=pltpu.VMEM),
        scratch_shapes=[
            pltpu.VMEM(tokens.shape, low),
            pltpu.VMEM(w_four.shape, low),
            pltpu.VMEM(w_gate.shape, low),
            pltpu.VMEM(w_back.shape, low),
            pltpu.VMEM(table.shape, low),
            pltpu.VMEM(group.shape, low),
            pltpu.VMEM((2,) + table.shape, low),
            pltpu.VMEM((groups, 4, length, GROUP_DIM), low),
            pltpu.VMEM((4, 2 * length, GROUP_DIM), low),
            pltpu.VMEM((2, length, GROUP_DIM), jnp.float32),
            pltpu.VMEM((groups, 4, length, GROUP_DIM), low),
            pltpu.VMEM((groups, length, GROUP_DIM), low),
            pltpu.VMEM((length, features), jnp.float32),
            pltpu.VMEM((length, features), jnp.float32),
            pltpu.SemaphoreType.DMA((5,)),
            pltpu.SemaphoreType.DMA((length // TILE,)),
            pltpu.SemaphoreType.DMA((groups, 2)),
            pltpu.SemaphoreType.DMA((groups, 4)),
            pltpu.SemaphoreType.DMA((groups,)),
            pltpu.SemaphoreType.DMA((groups,)),
            pltpu.SemaphoreType.DMA((groups, 4)),
            pltpu.SemaphoreType.DMA((groups, 4)),
        ],
        compiler_params=pltpu.CompilerParams(
            collective_id=0, has_side_effects=True, vmem_limit_bytes=60 * 1024 * 1024
        ),
    )(tokens, w_four, w_gate, w_back, table, group)


def solution(mesh):
    square = mesh.shape["row"] == 4 and mesh.shape["col"] == 4
    return jax.shard_map(
        on_line if square else on_device,
        mesh=mesh,
        in_specs=(P(("grp", "row"), None), P(None, "col"), P(None, "col"), P(None, "col")),
        out_specs=P(("grp", "row"), "col"),
        check_vma=False,
    )
```

```python
import functools
import math

import jax
import jax.numpy as jnp
import numpy as np
from jax import lax
from jax.experimental import pallas as pl
from jax.experimental.pallas import tpu as pltpu
from jax.sharding import PartitionSpec as P

GROUP_DIM = 128


def tables(count_len):
    steps = lax.iota(jnp.int32, count_len)
    product = steps[:, None] * steps[None, :] % count_len
    angles = product.astype(jnp.float32) * (2.0 * math.pi / count_len)
    return (jnp.cos(angles), jnp.sin(angles))


def channel_mix(values, matrix):
    height = values.shape[0]
    shaped = values.reshape(height, -1, GROUP_DIM)
    mixed_ch = jnp.einsum("ngc,cj->ngj", shaped, matrix, precision=lax.Precision.HIGHEST)
    return mixed_ch.reshape(height, -1)


def across_rows(values, matrix):
    return jnp.einsum("kr,rmc->kmc", matrix, values, precision=lax.Precision.HIGHEST)


def long_transform(col_re, col_im):
    length = col_re.shape[0]
    first_len = 8
    second_len = length // first_len
    shaped_re = col_re.reshape(first_len, second_len, -1)
    shaped_im = col_im.reshape(first_len, second_len, -1)
    cos_first, sin_first = tables(first_len)
    cos_second, sin_second = tables(second_len)
    section_re = across_rows(shaped_re, cos_first) + across_rows(shaped_im, sin_first)
    section_im = across_rows(shaped_im, cos_first) - across_rows(shaped_re, sin_first)
    outer = lax.iota(jnp.int32, first_len)[:, None]
    inner = lax.iota(jnp.int32, second_len)[None, :]
    angle = (outer * inner % length).astype(jnp.float32) * (2.0 * math.pi / length)
    turn_cos = jnp.cos(angle)[:, :, None]
    turn_sin = jnp.sin(angle)[:, :, None]
    bent_re = section_re * turn_cos + section_im * turn_sin
    bent_im = section_im * turn_cos - section_re * turn_sin
    final_re = jnp.einsum("qb,kbc->qkc", cos_second, bent_re, precision=lax.Precision.HIGHEST)
    final_re = final_re + jnp.einsum(
        "qb,kbc->qkc", sin_second, bent_im, precision=lax.Precision.HIGHEST
    )
    final_re = final_re.reshape(length, -1)
    final_im = jnp.einsum("qb,kbc->qkc", cos_second, bent_im, precision=lax.Precision.HIGHEST)
    final_im = final_im - jnp.einsum(
        "qb,kbc->qkc", sin_second, bent_re, precision=lax.Precision.HIGHEST
    )
    return (final_re, final_im.reshape(length, -1))


def on_device(tokens, w_four, w_gate, w_back):
    length = tokens.shape[0]
    row_count = lax.axis_size("row")
    row_index = lax.axis_index("row")
    piece_rows = length // row_count
    total_len = length * row_count
    feats = jnp.dot(tokens, w_four, preferred_element_type=jnp.float32).astype(jnp.bfloat16)
    lifted = feats.astype(jnp.float32)
    cos_group, sin_group = tables(GROUP_DIM)
    cos_rows, sin_rows = tables(row_count)
    residue = lax.iota(jnp.int32, row_count)[:, None]
    within = row_index * piece_rows + lax.iota(jnp.int32, piece_rows)[None, :]
    twist = (residue * within % total_len).astype(jnp.float32) * (2.0 * math.pi / total_len)
    twist_cos = jnp.cos(twist)[:, :, None]
    twist_sin = jnp.sin(twist)[:, :, None]
    line_re = lax.all_to_all(
        lifted[None].astype(jnp.bfloat16), "row", split_axis=1, concat_axis=0, tiled=True
    ).astype(jnp.float32)
    freq_re = across_rows(line_re, cos_rows)
    freq_im = -across_rows(line_re, sin_rows)
    turned_re = freq_re * twist_cos + freq_im * twist_sin
    turned_im = freq_im * twist_cos - freq_re * twist_sin
    col_re, col_im = (
        lax.all_to_all(turned_re, "row", split_axis=0, concat_axis=1, tiled=True),
        lax.all_to_all(turned_im, "row", split_axis=0, concat_axis=1, tiled=True),
    )
    col_re = col_re.reshape(length, -1)
    col_im = col_im.reshape(length, -1)
    whole_re, whole_im = long_transform(col_re, col_im)
    result = channel_mix(whole_re, cos_group) + channel_mix(whole_im, sin_group)
    scaled = (result * (1.0 / math.sqrt(total_len * GROUP_DIM))).astype(jnp.bfloat16)
    ordered = lax.all_to_all(scaled[:, None], "row", split_axis=0, concat_axis=1, tiled=True)
    ordered = ordered.reshape(length, -1)
    proj = jnp.dot(
        lax.all_gather(ordered, "col", axis=1, tiled=True),
        w_back,
        preferred_element_type=jnp.float32,
    )
    gate = jax.nn.sigmoid(jnp.dot(tokens, w_gate, preferred_element_type=jnp.float32))
    return (gate * proj).astype(jnp.bfloat16)


MESH = pl.DeviceIdType.MESH
TILE = 160


def position_table(length, row_count):
    place = np.arange(length)
    order = place.reshape(-1, row_count).T.reshape(-1)
    angle = 2.0 * np.pi * (np.outer(order, place) % (length * row_count)) / (length * row_count)
    table = np.concatenate([np.cos(angle), np.sin(angle)], axis=1)
    return table.reshape(row_count, length // row_count, 2 * length).astype(jnp.bfloat16)


def group_table():
    step = np.arange(GROUP_DIM)
    angle = 2.0 * np.pi * (np.outer(step, step) % GROUP_DIM) / GROUP_DIM
    return np.concatenate([np.cos(angle), np.sin(angle)], axis=1).astype(jnp.bfloat16)


def dot32(a, b):
    return jnp.dot(a, b, preferred_element_type=jnp.float32)


def mixing_kernel(
    tokens_hbm, four_hbm, gate_hbm, back_hbm, table_hbm, group_hbm, out_hbm,
    tokens, w_four, w_gate, w_back, table, group, turned, lines, spect, final, blocks, outer, gate, total, ready,
    load_sem, token_sem, line_send, line_recv, outer_send, outer_recv, col_send, col_recv, out_sem,
):
    row, col = lax.axis_index("row"), lax.axis_index("col")
    length = tokens.shape[0]
    quarter, half = length // 4, length // 2
    tiles = length // TILE
    groups = lines.shape[0]
    scale = 1.0 / math.sqrt(4 * length * GROUP_DIM)
    inner = jnp.logical_or(row == 1, row == 2)
    ends = jnp.logical_not(inner)
    end_row = 3 * (row // 2)
    sibling = col + 1 - 2 * (col % 2)
    across = col + 2 - 4 * (col // 2)
    opposite = across + 1 - 2 * (across % 2)

    loads = []
    for at, (source, target) in enumerate(
        ((four_hbm, w_four), (gate_hbm, w_gate), (table_hbm, table), (group_hbm, group), (back_hbm, w_back))
    ):
        loads.append(pltpu.make_async_copy(source, target, load_sem.at[at]))

    def tile_rows(tile):
        return pl.ds(pl.multiple_of(tile * TILE, TILE), TILE)

    def token_copy(tile):
        return pltpu.make_async_copy(tokens_hbm.at[tile_rows(tile), :], tokens.at[tile_rows(tile), :], token_sem.at[tile])

    loads[0].start()
    for tile in range(tiles):
        token_copy(tile).start()
    for load in loads[1:]:
        load.start()

    barrier = pltpu.get_barrier_semaphore()
    for step in (1, 2, 3):
        pl.semaphore_signal(barrier, inc=1, device_id={"row": (row + step) % 4}, device_id_type=MESH)
    for peer in (sibling, across):
        pl.semaphore_signal(barrier, inc=1, device_id={"col": peer}, device_id_type=MESH)

    def line_copy(g, part, origin, target, at):
        rows = pl.ds(part * half, half)
        return pltpu.make_async_remote_copy(
            src_ref=lines.at[g, origin, rows],
            dst_ref=lines.at[g, origin, rows],
            send_sem=line_send.at[at, g, part],
            recv_sem=line_recv.at[g, part, origin],
            device_id={"row": target},
            device_id_type=MESH,
        )

    near = 1 + row // 2
    own_target = jnp.where(inner, 3 - row, near)

    def feats(tile):
        values = dot32(tokens[tile_rows(tile), :], w_four[...]).astype(jnp.bfloat16)
        for g in range(groups):
            lines[g, row, tile_rows(tile), :] = values[:, g * GROUP_DIM : (g + 1) * GROUP_DIM]

    loads[0].wait()
    for part in range(2):

        @pl.loop(part * tiles // 2, (part + 1) * tiles // 2)
        def _(tile):
            token_copy(tile).wait()
            feats(tile)

        if part == 0:
            pl.semaphore_wait(barrier, 5)
        line_copy(0, part, row, own_target, 0).start()
    for g in range(1, groups):
        for part in range(2):
            line_copy(g, part, row, own_target, 0).start()

    loads[1].wait()

    @pl.loop(0, tiles)
    def _(tile):
        gate[tile_rows(tile), :] = jax.nn.sigmoid(dot32(tokens[tile_rows(tile), :], w_gate[...]))

    for load in loads[2:]:
        load.wait()

    def relay(g):
        for part in range(2):
            line_copy(g, part, end_row, 3 - row, 1).wait_recv()
            line_copy(g, part, end_row, 3 - row, 1).start()

    def turn_tables():
        for at, out_row in enumerate((end_row, row)):
            turn = out_row * lax.broadcasted_iota(jnp.int32, (quarter, length), 1) % 4
            odd, minus = turn % 2 == 1, jnp.where(turn >= 2, -1.0, 1.0)
            for s in range(4):
                cos_at = table[s, :, :length].astype(jnp.float32)
                sin_at = table[s, :, length:].astype(jnp.float32)
                turned_cos = jnp.where(odd, -sin_at, cos_at) * minus
                turned_sin = jnp.where(odd, cos_at, sin_at) * minus
                turned[at, s, :, :length] = turned_cos.astype(jnp.bfloat16)
                turned[at, s, :, length:] = (-turned_sin).astype(jnp.bfloat16)

    @pl.when(inner)
    def _():
        relay(0)
        turn_tables()
        for g in range(1, groups):
            relay(g)

    def outer_copy(g, part):
        rows = pl.ds(part * half, half)
        return pltpu.make_async_remote_copy(
            src_ref=outer.at[g, rows],
            dst_ref=blocks.at[g, 0, rows],
            send_sem=outer_send.at[g, part],
            recv_sem=outer_recv.at[g, part],
            device_id={"row": end_row},
            device_id_type=MESH,
        )

    def col_copy(g, part, source, slot, target):
        rows = pl.ds(part * half, half)
        return pltpu.make_async_remote_copy(
            src_ref=blocks.at[g, source, rows],
            dst_ref=blocks.at[g, slot, rows],
            send_sem=col_send.at[g, part, slot],
            recv_sem=col_recv.at[g, part, slot],
            device_id={"col": target},
            device_id_type=MESH,
        )

    def share_own(g, part):
        col_copy(g, part, 0, 2, across).start()
        col_copy(g, part, 0, 1, sibling).start()

    def transform(g):
        for part in range(2):
            for origin in (3 - row, 3 - end_row):
                line_copy(g, part, origin, 3 - row, 0).wait_recv()

            @pl.loop(part * tiles // 2, (part + 1) * tiles // 2)
            def _(tile):
                rows, low = tile_rows(tile), tile_rows(tiles + tile)
                x0, x1, x2, x3 = (lines[g, at, rows, :].astype(jnp.float32) for at in range(4))
                even, odd = x0 + x2, x1 + x3
                parts = (even + odd, x0 - x2, even - odd, x1 - x3)
                mixed = [dot32(value.astype(jnp.bfloat16), group[...]) for value in parts]
                cos_of = [value[:, :GROUP_DIM] for value in mixed]
                sin_of = [value[:, GROUP_DIM:] for value in mixed]
                for s in (0, 2):
                    spect[s, rows, :] = cos_of[s].astype(jnp.bfloat16)
                    spect[s, low, :] = sin_of[s].astype(jnp.bfloat16)
                spect[1, rows, :] = (cos_of[1] - sin_of[3]).astype(jnp.bfloat16)
                spect[1, low, :] = (sin_of[1] + cos_of[3]).astype(jnp.bfloat16)
                spect[3, rows, :] = (cos_of[1] + sin_of[3]).astype(jnp.bfloat16)
                spect[3, low, :] = (sin_of[1] - cos_of[3]).astype(jnp.bfloat16)

        for at in range(2):
            for part in range(2):
                rows = pl.ds(part * half, half)
                some = pl.ds(part * quarter // 2, quarter // 2)
                for s in range(4):
                    value = dot32(turned[at, s, some, :], spect[s]) * scale
                    final[at, pl.ds(part * half + s, quarter // 2, stride=4), :] = value
                if at == 0:
                    outer[g, rows, :] = final[at, rows, :].astype(jnp.bfloat16)
                    outer_copy(g, part).start()
                else:
                    blocks[g, 0, rows, :] = final[at, rows, :].astype(jnp.bfloat16)
                    share_own(g, part)

    def receive(g):
        for part in range(2):
            outer_copy(g, part).wait_recv()
            share_own(g, part)

    def back_rows(g, peer):
        return w_back[pl.ds(pl.multiple_of((peer * groups + g) * GROUP_DIM, GROUP_DIM), GROUP_DIM), :]

    def out_copy(part):
        rows = pl.ds(part * half, half)
        return pltpu.make_async_copy(ready.at[rows, :], out_hbm.at[rows, :], out_sem.at[part])

    def finish(g):
        for part in range(2):
            col_copy(g, part, 0, 1, sibling).wait_recv()

            @pl.loop(part * tiles // 2, (part + 1) * tiles // 2)
            def _(tile):
                rows = tile_rows(tile)
                share = dot32(blocks[g, 0, rows, :], back_rows(g, col))
                share = share + dot32(blocks[g, 1, rows, :], back_rows(g, sibling))
                total[rows, :] = share if g == 0 else total[rows, :] + share

        for part in range(2):
            col_copy(g, part, 0, 2, across).wait_recv()
            col_copy(g, part, 2, 3, sibling).start()
        for part in range(2):
            col_copy(g, part, 2, 3, sibling).wait_recv()

            @pl.loop(part * tiles // 2, (part + 1) * tiles // 2)
            def _(tile):
                rows = tile_rows(tile)
                share = dot32(blocks[g, 2, rows, :], back_rows(g, across))
                share = share + dot32(blocks[g, 3, rows, :], back_rows(g, opposite))
                summed = total[rows, :] + share
                if g < groups - 1:
                    total[rows, :] = summed
                else:
                    ready[rows, :] = (gate[rows, :] * summed).astype(jnp.bfloat16)

            if g == groups - 1:
                out_copy(part).start()

    @pl.when(inner)
    def _():
        for g in range(groups):
            transform(g)

    for g in range(groups):
        pl.when(ends)(functools.partial(receive, g))
        finish(g)

    for part in range(2):
        for g in range(groups):
            for slot in (1, 2, 3):
                col_copy(g, part, 0 if slot < 3 else 2, slot, sibling).wait_send()
            line_copy(g, part, row, own_target, 0).wait_send()
    for part in range(2):

        @pl.when(inner)
        def _():
            for g in range(groups):
                outer_copy(g, part).wait_send()
                line_copy(g, part, end_row, 3 - row, 1).wait_send()

        out_copy(part).wait()


def on_line(tokens, w_four, w_gate, w_back):
    length, width = tokens.shape
    groups = w_four.shape[1] // GROUP_DIM
    features = w_gate.shape[1]
    quarter = length // 4
    low = jnp.bfloat16
    table = jnp.asarray(position_table(length, 4))
    group = jnp.asarray(group_table())
    hbm = pl.BlockSpec(memory_space=pl.ANY)
    return pl.pallas_call(
        mixing_kernel,
        out_shape=jax.ShapeDtypeStruct((length, features), low),
        in_specs=[hbm] * 6,
        out_specs=hbm,
        scratch_shapes=[
            pltpu.VMEM(tokens.shape, low),
            pltpu.VMEM(w_four.shape, low),
            pltpu.VMEM(w_gate.shape, low),
            pltpu.VMEM(w_back.shape, low),
            pltpu.VMEM(table.shape, low),
            pltpu.VMEM(group.shape, low),
            pltpu.VMEM((2,) + table.shape, low),
            pltpu.VMEM((groups, 4, length, GROUP_DIM), low),
            pltpu.VMEM((4, 2 * length, GROUP_DIM), low),
            pltpu.VMEM((2, length, GROUP_DIM), jnp.float32),
            pltpu.VMEM((groups, 4, length, GROUP_DIM), low),
            pltpu.VMEM((groups, length, GROUP_DIM), low),
            pltpu.VMEM((length, features), jnp.float32),
            pltpu.VMEM((length, features), jnp.float32),
            pltpu.VMEM((length, features), low),
            pltpu.SemaphoreType.DMA((5,)),
            pltpu.SemaphoreType.DMA((length // TILE,)),
            pltpu.SemaphoreType.DMA((2, groups, 2)),
            pltpu.SemaphoreType.DMA((groups, 2, 4)),
            pltpu.SemaphoreType.DMA((groups, 2)),
            pltpu.SemaphoreType.DMA((groups, 2)),
            pltpu.SemaphoreType.DMA((groups, 2, 4)),
            pltpu.SemaphoreType.DMA((groups, 2, 4)),
            pltpu.SemaphoreType.DMA((2,)),
        ],
        compiler_params=pltpu.CompilerParams(
            collective_id=0, has_side_effects=True, vmem_limit_bytes=60 * 1024 * 1024
        ),
    )(tokens, w_four, w_gate, w_back, table, group)


def solution(mesh):
    square = mesh.shape["row"] == 4 and mesh.shape["col"] == 4
    return jax.shard_map(
        on_line if square else on_device,
        mesh=mesh,
        in_specs=(P(("grp", "row"), None), P(None, "col"), P(None, "col"), P(None, "col")),
        out_specs=P(("grp", "row"), "col"),
        check_vma=False,
    )
```

```python
import functools
import math

import jax
import jax.numpy as jnp
import numpy as np
from jax import lax
from jax.experimental import pallas as pl
from jax.experimental.pallas import tpu as pltpu
from jax.sharding import PartitionSpec as P

GROUP_DIM = 128


def tables(count_len):
    steps = lax.iota(jnp.int32, count_len)
    product = steps[:, None] * steps[None, :] % count_len
    angles = product.astype(jnp.float32) * (2.0 * math.pi / count_len)
    return (jnp.cos(angles), jnp.sin(angles))


def channel_mix(values, matrix):
    height = values.shape[0]
    shaped = values.reshape(height, -1, GROUP_DIM)
    mixed_ch = jnp.einsum("ngc,cj->ngj", shaped, matrix, precision=lax.Precision.HIGHEST)
    return mixed_ch.reshape(height, -1)


def across_rows(values, matrix):
    return jnp.einsum("kr,rmc->kmc", matrix, values, precision=lax.Precision.HIGHEST)


def long_transform(col_re, col_im):
    length = col_re.shape[0]
    first_len = 8
    second_len = length // first_len
    shaped_re = col_re.reshape(first_len, second_len, -1)
    shaped_im = col_im.reshape(first_len, second_len, -1)
    cos_first, sin_first = tables(first_len)
    cos_second, sin_second = tables(second_len)
    section_re = across_rows(shaped_re, cos_first) + across_rows(shaped_im, sin_first)
    section_im = across_rows(shaped_im, cos_first) - across_rows(shaped_re, sin_first)
    outer = lax.iota(jnp.int32, first_len)[:, None]
    inner = lax.iota(jnp.int32, second_len)[None, :]
    angle = (outer * inner % length).astype(jnp.float32) * (2.0 * math.pi / length)
    turn_cos = jnp.cos(angle)[:, :, None]
    turn_sin = jnp.sin(angle)[:, :, None]
    bent_re = section_re * turn_cos + section_im * turn_sin
    bent_im = section_im * turn_cos - section_re * turn_sin
    final_re = jnp.einsum("qb,kbc->qkc", cos_second, bent_re, precision=lax.Precision.HIGHEST)
    final_re = final_re + jnp.einsum(
        "qb,kbc->qkc", sin_second, bent_im, precision=lax.Precision.HIGHEST
    )
    final_re = final_re.reshape(length, -1)
    final_im = jnp.einsum("qb,kbc->qkc", cos_second, bent_im, precision=lax.Precision.HIGHEST)
    final_im = final_im - jnp.einsum(
        "qb,kbc->qkc", sin_second, bent_re, precision=lax.Precision.HIGHEST
    )
    return (final_re, final_im.reshape(length, -1))


def on_device(tokens, w_four, w_gate, w_back):
    length = tokens.shape[0]
    row_count = lax.axis_size("row")
    row_index = lax.axis_index("row")
    piece_rows = length // row_count
    total_len = length * row_count
    feats = jnp.dot(tokens, w_four, preferred_element_type=jnp.float32).astype(jnp.bfloat16)
    lifted = feats.astype(jnp.float32)
    cos_group, sin_group = tables(GROUP_DIM)
    cos_rows, sin_rows = tables(row_count)
    residue = lax.iota(jnp.int32, row_count)[:, None]
    within = row_index * piece_rows + lax.iota(jnp.int32, piece_rows)[None, :]
    twist = (residue * within % total_len).astype(jnp.float32) * (2.0 * math.pi / total_len)
    twist_cos = jnp.cos(twist)[:, :, None]
    twist_sin = jnp.sin(twist)[:, :, None]
    line_re = lax.all_to_all(
        lifted[None].astype(jnp.bfloat16), "row", split_axis=1, concat_axis=0, tiled=True
    ).astype(jnp.float32)
    freq_re = across_rows(line_re, cos_rows)
    freq_im = -across_rows(line_re, sin_rows)
    turned_re = freq_re * twist_cos + freq_im * twist_sin
    turned_im = freq_im * twist_cos - freq_re * twist_sin
    col_re, col_im = (
        lax.all_to_all(turned_re, "row", split_axis=0, concat_axis=1, tiled=True),
        lax.all_to_all(turned_im, "row", split_axis=0, concat_axis=1, tiled=True),
    )
    col_re = col_re.reshape(length, -1)
    col_im = col_im.reshape(length, -1)
    whole_re, whole_im = long_transform(col_re, col_im)
    result = channel_mix(whole_re, cos_group) + channel_mix(whole_im, sin_group)
    scaled = (result * (1.0 / math.sqrt(total_len * GROUP_DIM))).astype(jnp.bfloat16)
    ordered = lax.all_to_all(scaled[:, None], "row", split_axis=0, concat_axis=1, tiled=True)
    ordered = ordered.reshape(length, -1)
    proj = jnp.dot(
        lax.all_gather(ordered, "col", axis=1, tiled=True),
        w_back,
        preferred_element_type=jnp.float32,
    )
    gate = jax.nn.sigmoid(jnp.dot(tokens, w_gate, preferred_element_type=jnp.float32))
    return (gate * proj).astype(jnp.bfloat16)


MESH = pl.DeviceIdType.MESH
TILE = 160


def position_table(length, row_count):
    place = np.arange(length)
    order = place.reshape(-1, row_count).T.reshape(-1)
    angle = 2.0 * np.pi * (np.outer(order, place) % (length * row_count)) / (length * row_count)
    table = np.concatenate([np.cos(angle), np.sin(angle)], axis=1)
    return table.reshape(row_count, length // row_count, 2 * length).astype(jnp.bfloat16)


def group_table():
    step = np.arange(GROUP_DIM)
    angle = 2.0 * np.pi * (np.outer(step, step) % GROUP_DIM) / GROUP_DIM
    return np.concatenate([np.cos(angle), np.sin(angle)], axis=1).astype(jnp.bfloat16)


def dot32(a, b):
    return jnp.dot(a, b, preferred_element_type=jnp.float32)


def mixing_kernel(
    tokens_hbm, four_hbm, gate_hbm, back_hbm, table_hbm, group_hbm, out_hbm,
    tokens, w_four, w_gate, w_back, table, group, turned, lines, spect, final, blocks, outer, gate, total, ready,
    load_sem, token_sem, line_send, line_recv, outer_send, outer_recv, col_send, col_recv, out_sem,
):
    row, col = lax.axis_index("row"), lax.axis_index("col")
    length = tokens.shape[0]
    quarter, half = length // 4, length // 2
    tiles = length // TILE
    groups = lines.shape[0]
    scale = 1.0 / math.sqrt(4 * length * GROUP_DIM)
    inner = jnp.logical_or(row == 1, row == 2)
    ends = jnp.logical_not(inner)
    end_row = 3 * (row // 2)
    sibling = col + 1 - 2 * (col % 2)
    across = col + 2 - 4 * (col // 2)
    opposite = across + 1 - 2 * (across % 2)

    loads = []
    for at, (source, target) in enumerate(
        ((four_hbm, w_four), (gate_hbm, w_gate), (table_hbm, table), (group_hbm, group), (back_hbm, w_back))
    ):
        loads.append(pltpu.make_async_copy(source, target, load_sem.at[at]))

    def tile_rows(tile):
        return pl.ds(pl.multiple_of(tile * TILE, TILE), TILE)

    def token_copy(tile):
        return pltpu.make_async_copy(tokens_hbm.at[tile_rows(tile), :], tokens.at[tile_rows(tile), :], token_sem.at[tile])

    loads[0].start()
    for tile in range(tiles):
        token_copy(tile).start()
    barrier = pltpu.get_barrier_semaphore()
    for step in (1, 2, 3):
        pl.semaphore_signal(barrier, inc=1, device_id={"row": (row + step) % 4}, device_id_type=MESH)
    for peer in (sibling, across):
        pl.semaphore_signal(barrier, inc=1, device_id={"col": peer}, device_id_type=MESH)

    def line_copy(g, part, origin, target, at):
        rows = pl.ds(part * half, half)
        return pltpu.make_async_remote_copy(
            src_ref=lines.at[g, origin, rows],
            dst_ref=lines.at[g, origin, rows],
            send_sem=line_send.at[at, g, part],
            recv_sem=line_recv.at[g, part, origin],
            device_id={"row": target},
            device_id_type=MESH,
        )

    near = 1 + row // 2
    own_target = jnp.where(inner, 3 - row, near)

    def feats(tile):
        values = dot32(tokens[tile_rows(tile), :], w_four[...]).astype(jnp.bfloat16)
        for g in range(groups):
            lines[g, row, tile_rows(tile), :] = values[:, g * GROUP_DIM : (g + 1) * GROUP_DIM]

    loads[0].wait()
    for part in range(2):

        @pl.loop(part * tiles // 2, (part + 1) * tiles // 2)
        def _(tile):
            token_copy(tile).wait()
            feats(tile)

        if part == 0:
            pl.semaphore_wait(barrier, 5)
        line_copy(0, part, row, own_target, 0).start()
        if part == 0:
            for load in loads[1:]:
                load.start()
    for g in range(1, groups):
        line_copy(g, 0, row, own_target, 0).start()

    @pl.when(ends)
    def _():
        for g in range(1, groups):
            line_copy(g, 1, row, own_target, 0).start()

    loads[1].wait()

    @pl.loop(0, tiles)
    def _(tile):
        gate[tile_rows(tile), :] = jax.nn.sigmoid(dot32(tokens[tile_rows(tile), :], w_gate[...]))

    for load in loads[2:]:
        load.wait()

    def relay(g):
        for part in range(2):
            line_copy(g, part, end_row, 3 - row, 1).wait_recv()
            line_copy(g, part, end_row, 3 - row, 1).start()

    def turn_tables():
        for at, out_row in enumerate((end_row, row)):
            turn = out_row * lax.broadcasted_iota(jnp.int32, (quarter, length), 1) % 4
            odd, minus = turn % 2 == 1, jnp.where(turn >= 2, -1.0, 1.0)
            for s in range(4):
                cos_at = table[s, :, :length].astype(jnp.float32)
                sin_at = table[s, :, length:].astype(jnp.float32)
                turned_cos = jnp.where(odd, -sin_at, cos_at) * minus
                turned_sin = jnp.where(odd, cos_at, sin_at) * minus
                turned[at, s, :, :length] = turned_cos.astype(jnp.bfloat16)
                turned[at, s, :, length:] = (-turned_sin).astype(jnp.bfloat16)

    @pl.when(inner)
    def _():
        relay(0)
        for g in range(1, groups):
            line_copy(g, 1, row, own_target, 0).start()
        turn_tables()
        for g in range(1, groups):
            relay(g)

    def outer_copy(g, part):
        rows = pl.ds(part * half, half)
        return pltpu.make_async_remote_copy(
            src_ref=outer.at[g, rows],
            dst_ref=blocks.at[g, 0, rows],
            send_sem=outer_send.at[g, part],
            recv_sem=outer_recv.at[g, part],
            device_id={"row": end_row},
            device_id_type=MESH,
        )

    def col_copy(g, part, source, slot, target):
        rows = pl.ds(part * half, half)
        return pltpu.make_async_remote_copy(
            src_ref=blocks.at[g, source, rows],
            dst_ref=blocks.at[g, slot, rows],
            send_sem=col_send.at[g, part, slot],
            recv_sem=col_recv.at[g, part, slot],
            device_id={"col": target},
            device_id_type=MESH,
        )

    def share_own(g, part):
        col_copy(g, part, 0, 2, across).start()
        col_copy(g, part, 0, 1, sibling).start()

    def transform(g):
        for part in range(2):
            for origin in (3 - row, 3 - end_row):
                line_copy(g, part, origin, 3 - row, 0).wait_recv()

            @pl.loop(part * tiles // 2, (part + 1) * tiles // 2)
            def _(tile):
                rows, low = tile_rows(tile), tile_rows(tiles + tile)
                x0, x1, x2, x3 = (lines[g, at, rows, :].astype(jnp.float32) for at in range(4))
                even, odd = x0 + x2, x1 + x3
                parts = (even + odd, x0 - x2, even - odd, x1 - x3)
                mixed = [dot32(value.astype(jnp.bfloat16), group[...]) for value in parts]
                cos_of = [value[:, :GROUP_DIM] for value in mixed]
                sin_of = [value[:, GROUP_DIM:] for value in mixed]
                for s in (0, 2):
                    spect[s, rows, :] = cos_of[s].astype(jnp.bfloat16)
                    spect[s, low, :] = sin_of[s].astype(jnp.bfloat16)
                spect[1, rows, :] = (cos_of[1] - sin_of[3]).astype(jnp.bfloat16)
                spect[1, low, :] = (sin_of[1] + cos_of[3]).astype(jnp.bfloat16)
                spect[3, rows, :] = (cos_of[1] + sin_of[3]).astype(jnp.bfloat16)
                spect[3, low, :] = (sin_of[1] - cos_of[3]).astype(jnp.bfloat16)

        for at in range(2):
            for part in range(2):
                rows = pl.ds(part * half, half)
                some = pl.ds(part * quarter // 2, quarter // 2)
                for s in range(4):
                    value = dot32(turned[at, s, some, :], spect[s]) * scale
                    final[at, pl.ds(part * half + s, quarter // 2, stride=4), :] = value
                if at == 0:
                    outer[g, rows, :] = final[at, rows, :].astype(jnp.bfloat16)
                    outer_copy(g, part).start()
                else:
                    blocks[g, 0, rows, :] = final[at, rows, :].astype(jnp.bfloat16)
                    share_own(g, part)

    def receive(g):
        for part in range(2):
            outer_copy(g, part).wait_recv()
            share_own(g, part)

    def back_rows(g, peer):
        return w_back[pl.ds(pl.multiple_of((peer * groups + g) * GROUP_DIM, GROUP_DIM), GROUP_DIM), :]

    def out_copy(part):
        rows = pl.ds(part * half, half)
        return pltpu.make_async_copy(ready.at[rows, :], out_hbm.at[rows, :], out_sem.at[part])

    def finish(g):
        for part in range(2):
            col_copy(g, part, 0, 1, sibling).wait_recv()

            @pl.loop(part * tiles // 2, (part + 1) * tiles // 2)
            def _(tile):
                rows = tile_rows(tile)
                share = dot32(blocks[g, 0, rows, :], back_rows(g, col))
                share = share + dot32(blocks[g, 1, rows, :], back_rows(g, sibling))
                total[rows, :] = share if g == 0 else total[rows, :] + share

        for part in range(2):
            col_copy(g, part, 0, 2, across).wait_recv()
            col_copy(g, part, 2, 3, sibling).start()

            @pl.loop(part * tiles // 2, (part + 1) * tiles // 2)
            def _(tile):
                rows = tile_rows(tile)
                total[rows, :] += dot32(blocks[g, 2, rows, :], back_rows(g, across))

        for part in range(2):
            col_copy(g, part, 2, 3, sibling).wait_recv()

            @pl.loop(part * tiles // 2, (part + 1) * tiles // 2)
            def _(tile):
                rows = tile_rows(tile)
                summed = total[rows, :] + dot32(blocks[g, 3, rows, :], back_rows(g, opposite))
                if g < groups - 1:
                    total[rows, :] = summed
                else:
                    ready[rows, :] = (gate[rows, :] * summed).astype(jnp.bfloat16)

            if g == groups - 1:
                out_copy(part).start()

    @pl.when(inner)
    def _():
        for g in range(groups):
            transform(g)

    for g in range(groups):
        pl.when(ends)(functools.partial(receive, g))
        finish(g)

    for part in range(2):
        for g in range(groups):
            for slot in (1, 2, 3):
                col_copy(g, part, 0 if slot < 3 else 2, slot, sibling).wait_send()
            line_copy(g, part, row, own_target, 0).wait_send()
    for part in range(2):

        @pl.when(inner)
        def _():
            for g in range(groups):
                outer_copy(g, part).wait_send()
                line_copy(g, part, end_row, 3 - row, 1).wait_send()

        out_copy(part).wait()


def on_line(tokens, w_four, w_gate, w_back):
    length, width = tokens.shape
    groups = w_four.shape[1] // GROUP_DIM
    features = w_gate.shape[1]
    quarter = length // 4
    low = jnp.bfloat16
    table = jnp.asarray(position_table(length, 4))
    group = jnp.asarray(group_table())
    tokens, w_four, w_gate, w_back, table, group = (pltpu.with_memory_space_constraint(x, pltpu.HBM) for x in (tokens, w_four, w_gate, w_back, table, group))
    hbm = pl.BlockSpec(memory_space=pltpu.HBM)
    return pl.pallas_call(
        mixing_kernel,
        out_shape=jax.ShapeDtypeStruct((length, features), low),
        in_specs=[hbm] * 6,
        out_specs=pl.BlockSpec(memory_space=pl.ANY),
        scratch_shapes=[
            pltpu.VMEM(tokens.shape, low),
            pltpu.VMEM(w_four.shape, low),
            pltpu.VMEM(w_gate.shape, low),
            pltpu.VMEM(w_back.shape, low),
            pltpu.VMEM(table.shape, low),
            pltpu.VMEM(group.shape, low),
            pltpu.VMEM((2,) + table.shape, low),
            pltpu.VMEM((groups, 4, length, GROUP_DIM), low),
            pltpu.VMEM((4, 2 * length, GROUP_DIM), low),
            pltpu.VMEM((2, length, GROUP_DIM), jnp.float32),
            pltpu.VMEM((groups, 4, length, GROUP_DIM), low),
            pltpu.VMEM((groups, length, GROUP_DIM), low),
            pltpu.VMEM((length, features), jnp.float32),
            pltpu.VMEM((length, features), jnp.float32),
            pltpu.VMEM((length, features), low),
            pltpu.SemaphoreType.DMA((5,)),
            pltpu.SemaphoreType.DMA((length // TILE,)),
            pltpu.SemaphoreType.DMA((2, groups, 2)),
            pltpu.SemaphoreType.DMA((groups, 2, 4)),
            pltpu.SemaphoreType.DMA((groups, 2)),
            pltpu.SemaphoreType.DMA((groups, 2)),
            pltpu.SemaphoreType.DMA((groups, 2, 4)),
            pltpu.SemaphoreType.DMA((groups, 2, 4)),
            pltpu.SemaphoreType.DMA((2,)),
        ],
        compiler_params=pltpu.CompilerParams(
            collective_id=0, has_side_effects=True, vmem_limit_bytes=28 * 1024 * 1024
        ),
    )(tokens, w_four, w_gate, w_back, table, group)


def solution(mesh):
    square = mesh.shape["row"] == 4 and mesh.shape["col"] == 4
    return jax.shard_map(
        on_line if square else on_device,
        mesh=mesh,
        in_specs=(P(("grp", "row"), None), P(None, "col"), P(None, "col"), P(None, "col")),
        out_specs=P(("grp", "row"), "col"),
        check_vma=False,
    )
```

```python
import functools
import math

import jax
import jax.numpy as jnp
import numpy as np
from jax import lax
from jax.experimental import pallas as pl
from jax.experimental.pallas import tpu as pltpu
from jax.sharding import PartitionSpec as P

GROUP_DIM = 128


def tables(count_len):
    steps = lax.iota(jnp.int32, count_len)
    product = steps[:, None] * steps[None, :] % count_len
    angles = product.astype(jnp.float32) * (2.0 * math.pi / count_len)
    return (jnp.cos(angles), jnp.sin(angles))


def channel_mix(values, matrix):
    height = values.shape[0]
    shaped = values.reshape(height, -1, GROUP_DIM)
    mixed_ch = jnp.einsum("ngc,cj->ngj", shaped, matrix, precision=lax.Precision.HIGHEST)
    return mixed_ch.reshape(height, -1)


def across_rows(values, matrix):
    return jnp.einsum("kr,rmc->kmc", matrix, values, precision=lax.Precision.HIGHEST)


def long_transform(col_re, col_im):
    length = col_re.shape[0]
    first_len = 8
    second_len = length // first_len
    shaped_re = col_re.reshape(first_len, second_len, -1)
    shaped_im = col_im.reshape(first_len, second_len, -1)
    cos_first, sin_first = tables(first_len)
    cos_second, sin_second = tables(second_len)
    section_re = across_rows(shaped_re, cos_first) + across_rows(shaped_im, sin_first)
    section_im = across_rows(shaped_im, cos_first) - across_rows(shaped_re, sin_first)
    outer = lax.iota(jnp.int32, first_len)[:, None]
    inner = lax.iota(jnp.int32, second_len)[None, :]
    angle = (outer * inner % length).astype(jnp.float32) * (2.0 * math.pi / length)
    turn_cos = jnp.cos(angle)[:, :, None]
    turn_sin = jnp.sin(angle)[:, :, None]
    bent_re = section_re * turn_cos + section_im * turn_sin
    bent_im = section_im * turn_cos - section_re * turn_sin
    final_re = jnp.einsum("qb,kbc->qkc", cos_second, bent_re, precision=lax.Precision.HIGHEST)
    final_re = final_re + jnp.einsum(
        "qb,kbc->qkc", sin_second, bent_im, precision=lax.Precision.HIGHEST
    )
    final_re = final_re.reshape(length, -1)
    final_im = jnp.einsum("qb,kbc->qkc", cos_second, bent_im, precision=lax.Precision.HIGHEST)
    final_im = final_im - jnp.einsum(
        "qb,kbc->qkc", sin_second, bent_re, precision=lax.Precision.HIGHEST
    )
    return (final_re, final_im.reshape(length, -1))


def on_device(tokens, w_four, w_gate, w_back):
    length = tokens.shape[0]
    row_count = lax.axis_size("row")
    row_index = lax.axis_index("row")
    piece_rows = length // row_count
    total_len = length * row_count
    feats = jnp.dot(tokens, w_four, preferred_element_type=jnp.float32).astype(jnp.bfloat16)
    lifted = feats.astype(jnp.float32)
    cos_group, sin_group = tables(GROUP_DIM)
    cos_rows, sin_rows = tables(row_count)
    residue = lax.iota(jnp.int32, row_count)[:, None]
    within = row_index * piece_rows + lax.iota(jnp.int32, piece_rows)[None, :]
    twist = (residue * within % total_len).astype(jnp.float32) * (2.0 * math.pi / total_len)
    twist_cos = jnp.cos(twist)[:, :, None]
    twist_sin = jnp.sin(twist)[:, :, None]
    line_re = lax.all_to_all(
        lifted[None].astype(jnp.bfloat16), "row", split_axis=1, concat_axis=0, tiled=True
    ).astype(jnp.float32)
    freq_re = across_rows(line_re, cos_rows)
    freq_im = -across_rows(line_re, sin_rows)
    turned_re = freq_re * twist_cos + freq_im * twist_sin
    turned_im = freq_im * twist_cos - freq_re * twist_sin
    col_re, col_im = (
        lax.all_to_all(turned_re, "row", split_axis=0, concat_axis=1, tiled=True),
        lax.all_to_all(turned_im, "row", split_axis=0, concat_axis=1, tiled=True),
    )
    col_re = col_re.reshape(length, -1)
    col_im = col_im.reshape(length, -1)
    whole_re, whole_im = long_transform(col_re, col_im)
    result = channel_mix(whole_re, cos_group) + channel_mix(whole_im, sin_group)
    scaled = (result * (1.0 / math.sqrt(total_len * GROUP_DIM))).astype(jnp.bfloat16)
    ordered = lax.all_to_all(scaled[:, None], "row", split_axis=0, concat_axis=1, tiled=True)
    ordered = ordered.reshape(length, -1)
    proj = jnp.dot(
        lax.all_gather(ordered, "col", axis=1, tiled=True),
        w_back,
        preferred_element_type=jnp.float32,
    )
    gate = jax.nn.sigmoid(jnp.dot(tokens, w_gate, preferred_element_type=jnp.float32))
    return (gate * proj).astype(jnp.bfloat16)


MESH = pl.DeviceIdType.MESH
TILE = 160
PIECE = 128


def position_table(length, row_count):
    place = np.arange(length)
    order = place.reshape(-1, row_count).T.reshape(-1)
    angle = 2.0 * np.pi * (np.outer(order, place) % (length * row_count)) / (length * row_count)
    table = np.concatenate([np.cos(angle), np.sin(angle)], axis=1)
    return table.reshape(row_count, length // row_count, 2 * length).astype(jnp.bfloat16)


def group_table():
    step = np.arange(GROUP_DIM)
    angle = 2.0 * np.pi * (np.outer(step, step) % GROUP_DIM) / GROUP_DIM
    return np.concatenate([np.cos(angle), np.sin(angle)], axis=1).astype(jnp.bfloat16)


def dot32(a, b):
    return jnp.dot(a, b, preferred_element_type=jnp.float32)


def mixing_kernel(
    tokens_hbm, four_hbm, gate_hbm, back_hbm, table_hbm, group_hbm, out_hbm,
    tokens, w_four, w_gate, w_back, table, group, turned, lines, spect, final, blocks, outer, gate, total, ready,
    load_sem, token_sem, line_send, line_recv, outer_send, outer_recv, col_send, col_recv, out_sem,
):
    row, col = lax.axis_index("row"), lax.axis_index("col")
    length = tokens.shape[0]
    quarter, half = length // 4, length // 2
    tiles, pieces = length // TILE, length // PIECE
    groups = lines.shape[0]
    scale = 1.0 / math.sqrt(4 * length * GROUP_DIM)
    inner = jnp.logical_or(row == 1, row == 2)
    ends = jnp.logical_not(inner)
    end_row = 3 * (row // 2)
    sibling = col + 1 - 2 * (col % 2)
    across = col + 2 - 4 * (col // 2)
    opposite = across + 1 - 2 * (across % 2)

    loads = []
    for at, (source, target) in enumerate(
        ((four_hbm, w_four), (gate_hbm, w_gate), (table_hbm, table), (group_hbm, group), (back_hbm, w_back))
    ):
        loads.append(pltpu.make_async_copy(source, target, load_sem.at[at]))

    def tile_rows(tile):
        return pl.ds(pl.multiple_of(tile * TILE, TILE), TILE)

    def piece_rows(piece):
        return pl.ds(pl.multiple_of(piece * PIECE, PIECE), PIECE)

    def token_copy(tile):
        return pltpu.make_async_copy(tokens_hbm.at[tile_rows(tile), :], tokens.at[tile_rows(tile), :], token_sem.at[tile])

    loads[0].start()
    for tile in range(tiles):
        token_copy(tile).start()
    barrier = pltpu.get_barrier_semaphore()
    for step in (1, 2, 3):
        pl.semaphore_signal(barrier, inc=1, device_id={"row": (row + step) % 4}, device_id_type=MESH)
    for peer in (sibling, across):
        pl.semaphore_signal(barrier, inc=1, device_id={"col": peer}, device_id_type=MESH)

    def line_copy(g, part, origin, target, at):
        rows = pl.ds(part * half, half)
        return pltpu.make_async_remote_copy(
            src_ref=lines.at[g, origin, rows],
            dst_ref=lines.at[g, origin, rows],
            send_sem=line_send.at[at, g, part],
            recv_sem=line_recv.at[g, part, origin],
            device_id={"row": target},
            device_id_type=MESH,
        )

    near = 1 + row // 2
    own_target = jnp.where(inner, 3 - row, near)

    def feats(tile):
        values = dot32(tokens[tile_rows(tile), :], w_four[...]).astype(jnp.bfloat16)
        for g in range(groups):
            lines[g, row, tile_rows(tile), :] = values[:, g * GROUP_DIM : (g + 1) * GROUP_DIM]

    loads[0].wait()
    for part in range(2):

        @pl.loop(part * tiles // 2, (part + 1) * tiles // 2)
        def _(tile):
            token_copy(tile).wait()
            feats(tile)

        if part == 0:
            pl.semaphore_wait(barrier, 5)
        line_copy(0, part, row, own_target, 0).start()
        if part == 0:
            for load in loads[1:]:
                load.start()
    for g in range(1, groups):
        line_copy(g, 0, row, own_target, 0).start()

    @pl.when(ends)
    def _():
        for g in range(1, groups):
            line_copy(g, 1, row, own_target, 0).start()

    loads[1].wait()

    @pl.loop(0, tiles)
    def _(tile):
        gate[tile_rows(tile), :] = jax.nn.sigmoid(dot32(tokens[tile_rows(tile), :], w_gate[...]))

    for load in loads[2:]:
        load.wait()

    def relay(g):
        for part in range(2):
            line_copy(g, part, end_row, 3 - row, 1).wait_recv()
            line_copy(g, part, end_row, 3 - row, 1).start()

    def turn_tables():
        for at, out_row in enumerate((end_row, row)):
            turn = out_row * lax.broadcasted_iota(jnp.int32, (quarter, length), 1) % 4
            odd, minus = turn % 2 == 1, jnp.where(turn >= 2, -1.0, 1.0)
            for s in range(4):
                cos_at = table[s, :, :length].astype(jnp.float32)
                sin_at = table[s, :, length:].astype(jnp.float32)
                turned_cos = jnp.where(odd, -sin_at, cos_at) * minus
                turned_sin = jnp.where(odd, cos_at, sin_at) * minus
                turned[at, s, :, :length] = turned_cos.astype(jnp.bfloat16)
                turned[at, s, :, length:] = (-turned_sin).astype(jnp.bfloat16)

    @pl.when(inner)
    def _():
        relay(0)
        for g in range(1, groups):
            line_copy(g, 1, row, own_target, 0).start()
        turn_tables()
        for g in range(1, groups):
            relay(g)

    def outer_copy(g, part):
        rows = piece_rows(part)
        return pltpu.make_async_remote_copy(
            src_ref=outer.at[g, rows],
            dst_ref=blocks.at[g, 0, rows],
            send_sem=outer_send.at[g, part],
            recv_sem=outer_recv.at[g, part],
            device_id={"row": end_row},
            device_id_type=MESH,
        )

    def col_copy(g, part, source, slot, target):
        rows = piece_rows(part)
        return pltpu.make_async_remote_copy(
            src_ref=blocks.at[g, source, rows],
            dst_ref=blocks.at[g, slot, rows],
            send_sem=col_send.at[g, part, slot],
            recv_sem=col_recv.at[g, part, slot],
            device_id={"col": target},
            device_id_type=MESH,
        )

    def share_own(g, part):
        col_copy(g, part, 0, 2, across).start()
        col_copy(g, part, 0, 1, sibling).start()

    def transform(g):
        for part in range(2):
            for origin in (3 - row, 3 - end_row):
                line_copy(g, part, origin, 3 - row, 0).wait_recv()

            @pl.loop(part * tiles // 2, (part + 1) * tiles // 2)
            def _(tile):
                rows, low = tile_rows(tile), tile_rows(tiles + tile)
                x0, x1, x2, x3 = (lines[g, at, rows, :].astype(jnp.float32) for at in range(4))
                even, odd = x0 + x2, x1 + x3
                parts = (even + odd, x0 - x2, even - odd, x1 - x3)
                mixed = [dot32(value.astype(jnp.bfloat16), group[...]) for value in parts]
                cos_of = [value[:, :GROUP_DIM] for value in mixed]
                sin_of = [value[:, GROUP_DIM:] for value in mixed]
                for s in (0, 2):
                    spect[s, rows, :] = cos_of[s].astype(jnp.bfloat16)
                    spect[s, low, :] = sin_of[s].astype(jnp.bfloat16)
                spect[1, rows, :] = (cos_of[1] - sin_of[3]).astype(jnp.bfloat16)
                spect[1, low, :] = (sin_of[1] + cos_of[3]).astype(jnp.bfloat16)
                spect[3, rows, :] = (cos_of[1] + sin_of[3]).astype(jnp.bfloat16)
                spect[3, low, :] = (sin_of[1] - cos_of[3]).astype(jnp.bfloat16)

        for at in range(2):

            @pl.loop(0, pieces)
            def _(part):
                step = PIECE // 4
                some = pl.ds(pl.multiple_of(part * step, step), step)
                for s in range(4):
                    final[pl.ds(s, step, stride=4), :] = dot32(turned[at, s, some, :], spect[s]) * scale
                if at == 0:
                    outer[g, piece_rows(part), :] = final[...].astype(jnp.bfloat16)
                    outer_copy(g, part).start()
                else:
                    blocks[g, 0, piece_rows(part), :] = final[...].astype(jnp.bfloat16)
                    share_own(g, part)

    def receive(g):
        @pl.loop(0, pieces)
        def _(part):
            outer_copy(g, part).wait_recv()
            share_own(g, part)

    def back_rows(g, peer):
        return w_back[pl.ds(pl.multiple_of((peer * groups + g) * GROUP_DIM, GROUP_DIM), GROUP_DIM), :]

    def out_copy(part):
        rows = piece_rows(part)
        return pltpu.make_async_copy(ready.at[rows, :], out_hbm.at[rows, :], out_sem.at[part])

    def finish(g):
        @pl.loop(0, pieces)
        def _(part):
            rows = piece_rows(part)
            col_copy(g, part, 0, 1, sibling).wait_recv()
            share = dot32(blocks[g, 0, rows, :], back_rows(g, col))
            share = share + dot32(blocks[g, 1, rows, :], back_rows(g, sibling))
            total[rows, :] = share if g == 0 else total[rows, :] + share

        @pl.loop(0, pieces)
        def _(part):
            rows = piece_rows(part)
            col_copy(g, part, 0, 2, across).wait_recv()
            col_copy(g, part, 2, 3, sibling).start()
            total[rows, :] += dot32(blocks[g, 2, rows, :], back_rows(g, across))

        @pl.loop(0, pieces)
        def _(part):
            rows = piece_rows(part)
            col_copy(g, part, 2, 3, sibling).wait_recv()
            summed = total[rows, :] + dot32(blocks[g, 3, rows, :], back_rows(g, opposite))
            if g < groups - 1:
                total[rows, :] = summed
            else:
                ready[rows, :] = (gate[rows, :] * summed).astype(jnp.bfloat16)
                out_copy(part).start()

    @pl.when(inner)
    def _():
        for g in range(groups):
            transform(g)

    for g in range(groups):
        pl.when(ends)(functools.partial(receive, g))
        finish(g)

    for part in range(2):
        for g in range(groups):
            line_copy(g, part, row, own_target, 0).wait_send()

    @pl.loop(0, pieces)
    def _(part):
        for g in range(groups):
            for slot in (1, 2, 3):
                col_copy(g, part, 0 if slot < 3 else 2, slot, sibling).wait_send()
        out_copy(part).wait()

    @pl.when(inner)
    def _():
        for part in range(2):
            for g in range(groups):
                line_copy(g, part, end_row, 3 - row, 1).wait_send()

        @pl.loop(0, pieces)
        def _(part):
            for g in range(groups):
                outer_copy(g, part).wait_send()


def on_line(tokens, w_four, w_gate, w_back):
    length, width = tokens.shape
    groups = w_four.shape[1] // GROUP_DIM
    features = w_gate.shape[1]
    pieces = length // PIECE
    low = jnp.bfloat16
    table = jnp.asarray(position_table(length, 4))
    group = jnp.asarray(group_table())
    tokens, w_four, w_gate, w_back, table, group = (
        pltpu.with_memory_space_constraint(x, pltpu.HBM) for x in (tokens, w_four, w_gate, w_back, table, group)
    )
    hbm = pl.BlockSpec(memory_space=pltpu.HBM)
    return pl.pallas_call(
        mixing_kernel,
        out_shape=jax.ShapeDtypeStruct((length, features), low),
        in_specs=[hbm] * 6,
        out_specs=pl.BlockSpec(memory_space=pl.ANY),
        scratch_shapes=[
            pltpu.VMEM(tokens.shape, low),
            pltpu.VMEM(w_four.shape, low),
            pltpu.VMEM(w_gate.shape, low),
            pltpu.VMEM(w_back.shape, low),
            pltpu.VMEM(table.shape, low),
            pltpu.VMEM(group.shape, low),
            pltpu.VMEM((2,) + table.shape, low),
            pltpu.VMEM((groups, 4, length, GROUP_DIM), low),
            pltpu.VMEM((4, 2 * length, GROUP_DIM), low),
            pltpu.VMEM((PIECE, GROUP_DIM), jnp.float32),
            pltpu.VMEM((groups, 4, length, GROUP_DIM), low),
            pltpu.VMEM((groups, length, GROUP_DIM), low),
            pltpu.VMEM((length, features), jnp.float32),
            pltpu.VMEM((length, features), jnp.float32),
            pltpu.VMEM((length, features), low),
            pltpu.SemaphoreType.DMA((5,)),
            pltpu.SemaphoreType.DMA((length // TILE,)),
            pltpu.SemaphoreType.DMA((2, groups, 2)),
            pltpu.SemaphoreType.DMA((groups, 2, 4)),
            pltpu.SemaphoreType.DMA((groups, pieces)),
            pltpu.SemaphoreType.DMA((groups, pieces)),
            pltpu.SemaphoreType.DMA((groups, pieces, 4)),
            pltpu.SemaphoreType.DMA((groups, pieces, 4)),
            pltpu.SemaphoreType.DMA((pieces,)),
        ],
        compiler_params=pltpu.CompilerParams(
            collective_id=0, has_side_effects=True, vmem_limit_bytes=28 * 1024 * 1024
        ),
    )(tokens, w_four, w_gate, w_back, table, group)


def solution(mesh):
    square = mesh.shape["row"] == 4 and mesh.shape["col"] == 4
    return jax.shard_map(
        on_line if square else on_device,
        mesh=mesh,
        in_specs=(P(("grp", "row"), None), P(None, "col"), P(None, "col"), P(None, "col")),
        out_specs=P(("grp", "row"), "col"),
        check_vma=False,
    )
```
